32 devices in a mesh: ep: 8 (over z, y), tp: 4 (over x, core).
Axes of the slice: x: 2, y: 2, z: 4, core: 2. Of those that a mesh axis runs over, the one named last changes fastest.
Arguments:
- tokens: bfloat16 [384, 2048], P(('ep', 'tp')), may hold values from -6 to 6
- cache_latent: bfloat16 [384, 1024, 512], P(('ep', 'tp')), may hold values from -1700 to 1700
- cache_rope: bfloat16 [384, 64, 1024], P(('ep', 'tp')), may hold values from -6 to 6
- lengths: int32 [384], P(('ep', 'tp')), may hold values from 128 to 1023, as said below
- attn_gain: bfloat16 [2048], replicated, may hold values from 0.099609375 to 1.8984375
- latent_gain: bfloat16 [512], replicated, may hold values from 0.099609375 to 1.8984375
- post_attn_gain: bfloat16 [2048], replicated, may hold values from 0.099609375 to 1.8984375
- ffn_gain: bfloat16 [2048], replicated, may hold values from 0.099609375 to 1.8984375
- post_ffn_gain: bfloat16 [2048], replicated, may hold values from 0.099609375 to 1.8984375
- w_query: bfloat16 [2048, 2048], P(None, 'tp'), may hold values from -0.125 to 0.125
- w_query_rot: bfloat16 [2048, 1024], P(None, 'tp'), may hold values from -0.125 to 0.125
- w_latent: bfloat16 [2048, 512], P(None, 'tp'), may hold values from -0.125 to 0.125
- w_key_rot: bfloat16 [2048, 64], replicated, may hold values from -0.125 to 0.125
- w_key_up: bfloat16 [512, 16, 128], P(None, 'tp'), may hold values from -0.25 to 0.25
- w_value_up: bfloat16 [512, 16, 128], P(None, 'tp'), may hold values from -0.25 to 0.25
- w_out: bfloat16 [2048, 2048], P('tp'), may hold values from -0.125 to 0.125
- route_logits: float32 [384, 4], P('ep'), may hold values from -6 to 6
- routes: int32 [384, 4], P('ep'), may hold values from 0 to 7, all different within a row; in each aligned block of 48 rows (0 to 47, 48 to 95, ...) at most 25 rows name the same one
- w_gate: bfloat16 [8, 2048, 2048], P('ep', None, 'tp'), may hold values from -0.3125 to 0.3125
- w_up: bfloat16 [8, 2048, 2048], P('ep', None, 'tp'), may hold values from -0.3125 to 0.3125
- w_down: bfloat16 [8, 2048, 2048], P('ep', 'tp'), may hold values from -0.125 to 0.125
Outputs:
- result: bfloat16 [384, 2048], P(('ep', 'tp'))
- new_latent: bfloat16 [384, 512], P(('ep', 'tp'))
- new_rope: bfloat16 [384, 64], P(('ep', 'tp'))
The draws below stay inside these ranges and needn't reach their ends.
Inputs may be any that keep to these rules, and one draw needn't show every extreme that they name: Each sequence's cache holds positions 0 to lengths - 1, and the new token stands at position lengths; some sequence has 1023 in every draw. `routes`: each row names 4 different experts; in each aligned block of 48 rows (the tokens of one index of ep) no expert is named more than 25 times, a bound that some block reaches.
All inputs are finite; a program needn't handle non-finite values.
Results may differ from the reference program's by a relative error of at most 0.019.
Values may be sent and summed in bfloat16 or wider, within the bound.
No kernel may reach another device: no remote copies, remote signals or barrier semaphores. Data moves between devices by JAX's collectives and lax.ppermute only.
A program may use at most 128 MiB of HBM per device.

```python
import math
import jax
import jax.numpy as jnp
import numpy as np
from jax import lax

D = 2048
HEADS = 16
KEY_DIM = 128
ROT_DIM = 64
VAL_DIM = 128
LATENT = 512
FF = 2048
TOP_K = 4
SEQ_DEV = 12
LEN = 1024
EXPERTS = 8
GROUP = 48
BATCH = 384
CAP = 25
N_TP = 4


def draw_cache_latent(key, part):
    base_key = jax.random.fold_in(jax.random.fold_in(key, 11), 0)
    cache = jnp.clip(jax.random.normal(base_key, (BATCH, LEN, LATENT), jnp.float32), -5.0, 5.0)
    return cache.astype(jnp.bfloat16)


def draw_lengths(key, part):
    keys = jax.random.split(jax.random.fold_in(key, 23), 3)
    lowest = LEN // 8
    ceilings = jax.random.randint(keys[0], (BATCH // SEQ_DEV,), LEN // 4, LEN)
    ceilings = jnp.repeat(ceilings, SEQ_DEV)
    drawn = jax.random.randint(keys[1], (BATCH,), lowest, ceilings)
    longest = jax.random.randint(keys[2], (), 0, BATCH)
    return jnp.where(jnp.arange(BATCH) == longest, LEN - 1, drawn).astype(jnp.int32)


def block_levels(rng, shape, cuts, least, top_value):
    def one(position, shards_of):
        heights = jax.random.uniform(jax.random.fold_in(jax.random.fold_in(rng, 6), position), (shards_of,), jnp.float32, least / len(cuts), top_value / len(cuts))
        return jnp.repeat(jnp.exp(heights), shape[position] // shards_of).reshape((-1,) + (1,) * (len(shape) - position - 1))

    loudness = one(*cuts[0])
    for cut in cuts[1:]:
        loudness = loudness * one(*cut)
    return loudness


def assign_block(stream_key, own, number, rows, count, top, limit, lean):
    order = jax.random.permutation(stream_key, count)
    heavy_load, ordinary = shares(count, rows * top, limit, lean, True), shares(count, rows * top, limit, lean, False)
    places = jnp.arange(count)

    def named(sizes, offset_by):
        used = int((sizes > 0).sum())
        fixed = max(1, used // 4)
        shifted = fixed + (places - fixed + offset_by * (used - fixed)) % max(1, count - fixed)
        return jnp.zeros((count,), jnp.int32).at[order[jnp.where(places < fixed, places, shifted)]].set(jnp.asarray(sizes, jnp.int32))

    sizes = jnp.where(number % 4 == 0, named(heavy_load, number // 4), named(ordinary, number - number // 4 - 1))
    mixed = jax.random.permutation(jax.random.fold_in(own, 3), count)
    source_of, sink = mixed[0:count // 2 * 2:2], mixed[1:count // 2 * 2:2]
    room = jnp.minimum(sizes[source_of] - 1, limit - sizes[sink]) // 2
    room = jnp.where((source_of == order[0]) | (sink == order[0]) | (sizes[sink] == 0), 0, jnp.maximum(room, 0))
    shifted = jax.random.randint(jax.random.fold_in(own, 4), (count // 2,), 0, 1 << 20) % (room + 1)
    sizes = sizes.at[source_of].add(-shifted).at[sink].add(shifted)
    members = jnp.searchsorted(jnp.cumsum(sizes), jnp.arange(rows * top), side="right").astype(jnp.int32)
    table = members.reshape(top, rows).T
    table = table[jax.random.permutation(jax.random.fold_in(own, 1), rows)]
    offset_by = jax.random.randint(jax.random.fold_in(own, 2), (rows, 1), 0, top)
    return jnp.take_along_axis(table, (jnp.arange(top)[None, :] + offset_by) % top, axis=1)


def shares(number_of, total, bound, slope, full):
    loads = [(1 << 20) // math.isqrt(grade ** slope) + 1 for grade in range(1, number_of + 1)]
    largest = bound if full else min(bound, max(-(-total // number_of), total * loads[0] // sum(loads)))
    least = 1 if total - largest >= number_of - 1 else 0
    given, rest = [largest] + [least] * (number_of - 1), total - largest - least * (number_of - 1)
    while rest > 0:
        free = [i for i in range(1, number_of) if given[i] < largest] or [i for i in range(1, number_of) if given[i] < bound]
        pool, budget = sum([loads[i] for i in free]), rest
        for i in free:
            addition = min(bound - given[i], max(1, budget * loads[i] // pool), rest)
            given[i] = given[i] + addition
            rest = rest - addition
    return np.array(given)


def bell_draw(key, shape, scale, most, cuts=(), kind=jnp.bfloat16):
    values = scale * jax.random.normal(key, shape, jnp.float32)
    if cuts:
        values = values * block_levels(key, shape, cuts, -0.22, 0.18)
    return jnp.clip(values, -most, most).astype(kind)


def setup_inputs(seed: int = 0) -> dict:
    key_list = jax.random.split(jax.random.key(seed), 22)
    tokens = bell_draw(key_list[0], (BATCH, D), 1.0, 6.0, ((0, 32),))
    cache_latent = draw_cache_latent(jax.random.fold_in(key_list[21], 71), 0)
    cache_rope = bell_draw(key_list[2], (BATCH, ROT_DIM, LEN), 1.0, 6.0, ((0, 32),))
    lengths = draw_lengths(jax.random.fold_in(key_list[21], 71), 0)
    attn_gain = jnp.clip(1.0 + 0.18 * jax.random.normal(key_list[4], (D,), jnp.float32), 0.099609375, 1.8984375).astype(jnp.bfloat16)
    latent_gain = jnp.clip(1.0 + 0.18 * jax.random.normal(key_list[5], (LATENT,), jnp.float32), 0.099609375, 1.8984375).astype(jnp.bfloat16)
    post_attn_gain = jnp.clip(1.0 + 0.18 * jax.random.normal(key_list[6], (D,), jnp.float32), 0.099609375, 1.8984375).astype(jnp.bfloat16)
    ffn_gain = jnp.clip(1.0 + 0.18 * jax.random.normal(key_list[7], (D,), jnp.float32), 0.099609375, 1.8984375).astype(jnp.bfloat16)
    post_ffn_gain = jnp.clip(1.0 + 0.18 * jax.random.normal(key_list[8], (D,), jnp.float32), 0.099609375, 1.8984375).astype(jnp.bfloat16)
    w_query = bell_draw(key_list[9], (D, HEADS * KEY_DIM), D ** -0.5, 0.125, ((1, 4),))
    w_query_rot = bell_draw(key_list[10], (D, HEADS * ROT_DIM), D ** -0.5, 0.125, ((1, 4),))
    w_latent = bell_draw(key_list[11], (D, LATENT), D ** -0.5, 0.125, ((1, 4),))
    w_key_rot = bell_draw(key_list[12], (D, ROT_DIM), D ** -0.5, 0.125)
    w_key_up = bell_draw(key_list[13], (LATENT, HEADS, KEY_DIM), LATENT ** -0.5, 0.25, ((1, 4),))
    w_value_up = bell_draw(key_list[14], (LATENT, HEADS, VAL_DIM), LATENT ** -0.5, 0.25, ((1, 4),))
    w_out = bell_draw(key_list[15], (HEADS * VAL_DIM, D), (HEADS * VAL_DIM) ** -0.5, 0.125, ((0, 4),))
    route_logits = bell_draw(key_list[16], (BATCH, TOP_K), 1.0, 6.0, ((0, 8),), jnp.float32)
    routes_keys = jax.random.split(jax.random.fold_in(key_list[17], 1), BATCH // GROUP)
    routes_turns = jax.random.permutation(jax.random.fold_in(key_list[17], 3), BATCH // GROUP)
    routes = jax.vmap(lambda own, number: assign_block(jax.random.fold_in(key_list[17], 2), own, number, GROUP, EXPERTS, TOP_K, CAP, 2))(routes_keys, routes_turns).reshape((BATCH, TOP_K))
    w_gate = bell_draw(key_list[18], (EXPERTS, D, FF), 0.055, 0.3125, ((0, 8), (2, 4)))
    w_up = bell_draw(key_list[19], (EXPERTS, D, FF), 0.055, 0.3125, ((0, 8), (2, 4)))
    w_down = bell_draw(key_list[20], (EXPERTS, FF, D), FF ** -0.5, 0.125, ((0, 8), (1, 4)))
    return dict(tokens=tokens, cache_latent=cache_latent, cache_rope=cache_rope, lengths=lengths, attn_gain=attn_gain, latent_gain=latent_gain, post_attn_gain=post_attn_gain, ffn_gain=ffn_gain, post_ffn_gain=post_ffn_gain, w_query=w_query, w_query_rot=w_query_rot, w_latent=w_latent, w_key_rot=w_key_rot, w_key_up=w_key_up, w_value_up=w_value_up, w_out=w_out, route_logits=route_logits, routes=routes, w_gate=w_gate, w_up=w_up, w_down=w_down)


eps_norm = 1e-06
clamp_limit = 7.0
sigmoid_alpha = 1.702
theta_base = 10000.0

def rms_scale(values, gain):
    mean_square = lax.optimization_barrier(jnp.mean(values * values, axis=-1, keepdims=True))
    return values * lax.rsqrt(mean_square + eps_norm) * gain.astype(jnp.float32)

def rotate(values, positions):
    half = values.shape[-1] // 2
    freqs = theta_base ** (-jnp.arange(half, dtype=jnp.float32) / half)
    angles = positions[..., None] * freqs
    cosine = jnp.cos(angles)
    sine = jnp.sin(angles)
    first = values[..., :half]
    second = values[..., half:]
    return jnp.concatenate([first * cosine - second * sine, second * cosine + first * sine], axis=-1)

def reference(tokens, cache_latent, cache_rope, lengths, attn_gain, latent_gain, post_attn_gain, ffn_gain, post_ffn_gain, w_query, w_query_rot, w_latent, w_key_rot, w_key_up, w_value_up, w_out, route_logits, routes, w_gate, w_up, w_down):
    batch, width = tokens.shape
    latent_size, heads, key_size = w_key_up.shape
    rot_size = w_key_rot.shape[1]
    value_size = w_value_up.shape[2]
    span = cache_latent.shape[1]
    scale = (key_size + rot_size) ** (-0.5)
    token_values = tokens.astype(jnp.float32)
    normed = rms_scale(token_values, attn_gain).astype(jnp.bfloat16)
    query_plain = jnp.dot(normed, w_query, preferred_element_type=jnp.float32).astype(jnp.bfloat16)
    query_plain = query_plain.reshape(batch, heads, key_size)
    query_rotary = jnp.dot(normed, w_query_rot, preferred_element_type=jnp.float32).astype(jnp.bfloat16)
    query_rotary = query_rotary.reshape(batch, heads, rot_size)
    latent_raw = jnp.dot(normed, w_latent, preferred_element_type=jnp.float32).astype(jnp.bfloat16)
    key_raw = jnp.dot(normed, w_key_rot, preferred_element_type=jnp.float32).astype(jnp.bfloat16)
    new_latent = rms_scale(latent_raw.astype(jnp.float32), latent_gain).astype(jnp.bfloat16)
    positions = lengths.astype(jnp.float32)
    new_rope = rotate(key_raw.astype(jnp.float32), positions).astype(jnp.bfloat16)
    query_turned = rotate(query_rotary.astype(jnp.float32), positions[:, None]).astype(jnp.bfloat16)
    query_latent = jnp.einsum('bhn,chn->bhc', query_plain.astype(jnp.float32), w_key_up.astype(jnp.float32)).astype(jnp.bfloat16)

    def attend(pieces):
        q_lat, q_turn, latents, rotary, fresh_latent, fresh_rope, length = pieces
        latents_f = latents.astype(jnp.float32)
        scores = jnp.einsum('hc,pc->hp', q_lat.astype(jnp.float32), latents_f)
        scores = (scores + jnp.einsum('hr,rp->hp', q_turn.astype(jnp.float32), rotary.astype(jnp.float32))) * scale
        self_score = (lax.optimization_barrier(jnp.sum(q_lat.astype(jnp.float32) * fresh_latent.astype(jnp.float32)[None, :], axis=-1)) + lax.optimization_barrier(jnp.sum(q_turn.astype(jnp.float32) * fresh_rope.astype(jnp.float32)[None, :], axis=-1))) * scale
        valid = jnp.arange(span, dtype=jnp.int32) < length
        masked = jnp.where(valid[None, :], scores, -jnp.inf)
        highest = jnp.maximum(lax.optimization_barrier(jnp.max(masked, axis=-1)), self_score)
        raised = jnp.exp(masked - highest[:, None])
        raised_self = jnp.exp(self_score - highest)
        total = lax.optimization_barrier(jnp.sum(raised, axis=-1)) + raised_self
        probs = (raised / total[:, None]).astype(jnp.bfloat16)
        prob_self = (raised_self / total).astype(jnp.bfloat16)
        summed = jnp.einsum('hp,pc->hc', probs.astype(jnp.float32), latents_f)
        summed = summed + prob_self.astype(jnp.float32)[:, None] * fresh_latent.astype(jnp.float32)[None, :]
        return summed.astype(jnp.bfloat16)
    head_latent = lax.map(attend, (query_latent, query_turned, cache_latent, cache_rope, new_latent, new_rope, lengths))
    values = jnp.einsum('bhc,chv->bhv', head_latent.astype(jnp.float32), w_value_up.astype(jnp.float32)).astype(jnp.bfloat16)
    flat_values = values.reshape(batch, heads * value_size)
    group_cols = heads // N_TP * value_size
    attn = jnp.zeros((batch, width), jnp.float32)
    for section in range(N_TP):
        lower = section * group_cols
        partial_sum = jnp.dot(flat_values[:, lower:lower + group_cols], w_out[lower:lower + group_cols], preferred_element_type=jnp.float32).astype(jnp.bfloat16)
        attn = attn + partial_sum.astype(jnp.float32)
    attn = attn.astype(jnp.bfloat16)
    mixed = (token_values + rms_scale(attn.astype(jnp.float32), post_attn_gain)).astype(jnp.bfloat16)
    ffn_input = rms_scale(mixed.astype(jnp.float32), ffn_gain).astype(jnp.bfloat16)
    route_weights = jax.nn.softmax(route_logits, axis=-1)
    top_k = routes.shape[1]
    experts = w_gate.shape[0]
    hidden = w_gate.shape[2]
    n_blocks = batch // GROUP
    assigned = GROUP * top_k
    flat_routes = routes.reshape(n_blocks, assigned).astype(jnp.int32)
    onehot = (flat_routes[:, :, None] == jnp.arange(experts, dtype=jnp.int32)[None, None, :]).astype(jnp.int32)
    rank = lax.optimization_barrier(jnp.sum((jnp.cumsum(onehot, axis=1) - onehot) * onehot, axis=-1)).astype(jnp.int32)
    block_ids = jnp.broadcast_to(jnp.arange(n_blocks, dtype=jnp.int32)[:, None], (n_blocks, assigned))
    token_ids = (jnp.arange(assigned, dtype=jnp.int32) // top_k).astype(jnp.int32)
    rows_in = ffn_input.reshape(n_blocks, GROUP, width)
    gathered = rows_in[:, token_ids]
    slots = jnp.zeros((n_blocks, experts, CAP, width), jnp.bfloat16).at[block_ids, flat_routes, rank].set(gathered)
    block_hidden = hidden // N_TP

    def expert(pieces):
        rows, gate_weight, up_weight, down_weight = pieces
        flat = rows.reshape(-1, width)
        gate = jnp.minimum(jnp.dot(flat, gate_weight, preferred_element_type=jnp.float32), clamp_limit)
        upward = jnp.clip(jnp.dot(flat, up_weight, preferred_element_type=jnp.float32), -clamp_limit, clamp_limit)
        active = ((upward + 1.0) * gate * jax.nn.sigmoid(sigmoid_alpha * gate)).astype(jnp.bfloat16)
        total = jnp.zeros((flat.shape[0], width), jnp.float32)
        for section in range(N_TP):
            lower = section * block_hidden
            piece = jnp.dot(active[:, lower:lower + block_hidden], down_weight[lower:lower + block_hidden], preferred_element_type=jnp.float32).astype(jnp.bfloat16)
            total = total + piece.astype(jnp.float32)
        return total.astype(jnp.bfloat16).reshape(rows.shape)
    outputs = lax.map(expert, (jnp.moveaxis(slots, 1, 0), w_gate, w_up, w_down))
    picked = outputs[flat_routes, block_ids, rank].astype(jnp.float32).reshape(batch, top_k, width)
    moe = lax.optimization_barrier(jnp.sum(picked * route_weights[:, :, None], axis=1)).astype(jnp.bfloat16)
    result = (mixed.astype(jnp.float32) + rms_scale(moe.astype(jnp.float32), post_ffn_gain)).astype(jnp.bfloat16)
    return (result, new_latent, new_rope)
```

```python
import jax
import jax.numpy as jnp
from jax import lax
from jax.sharding import PartitionSpec as P

eps_norm = 1e-06
clamp_limit = 7.0
sigmoid_alpha = 1.702
theta_base = 10000.0


def rms_scale(values, gain):
    mean_square = jnp.mean(values * values, axis=-1, keepdims=True)
    return values * lax.rsqrt(mean_square + eps_norm) * gain.astype(jnp.float32)


def rotate(values, positions):
    half = values.shape[-1] // 2
    freqs = theta_base ** (-jnp.arange(half, dtype=jnp.float32) / half)
    angles = positions[..., None] * freqs
    cosine = jnp.cos(angles)
    sine = jnp.sin(angles)
    first = values[..., :half]
    second = values[..., half:]
    return jnp.concatenate(
        [first * cosine - second * sine, second * cosine + first * sine], axis=-1
    )


def attend(
    query_latent, query_turned, cache_latent, cache_rope, new_latent, new_rope, lengths, scale
):
    sequences, heads, latent_size = query_latent.shape
    span = cache_latent.shape[1]
    stride = min(512, span)
    blocks_used = (jnp.max(lengths) + stride - 1) // stride

    def score_block(index, scores):
        offset = index * stride
        latents = lax.dynamic_slice_in_dim(cache_latent, offset, stride, 1)
        rotary = lax.dynamic_slice_in_dim(cache_rope, offset, stride, 2)
        block_scores = jnp.einsum(
            "shc,spc->shp", query_latent, latents, preferred_element_type=jnp.float32
        )
        block_scores = block_scores + jnp.einsum(
            "shr,srp->shp", query_turned, rotary, preferred_element_type=jnp.float32
        )
        return lax.dynamic_update_slice_in_dim(scores, block_scores * scale, offset, 2)

    scores = lax.fori_loop(
        0, blocks_used, score_block, jnp.zeros((sequences, heads, span), jnp.float32)
    )
    self_score = (
        jnp.einsum("shc,sc->sh", query_latent, new_latent, preferred_element_type=jnp.float32)
        + jnp.einsum("shr,sr->sh", query_turned, new_rope, preferred_element_type=jnp.float32)
    ) * scale
    valid = jnp.arange(span, dtype=jnp.int32)[None, None, :] < lengths[:, None, None]
    masked = jnp.where(valid, scores, -jnp.inf)
    highest = jnp.maximum(jnp.max(masked, axis=-1), self_score)
    raised = jnp.exp(masked - highest[..., None])
    raised_self = jnp.exp(self_score - highest)
    total = jnp.sum(raised, axis=-1) + raised_self
    probs = (raised / total[..., None]).astype(jnp.bfloat16)
    prob_self = (raised_self / total).astype(jnp.bfloat16)

    def read_block(index, summed):
        offset = index * stride
        latents = lax.dynamic_slice_in_dim(cache_latent, offset, stride, 1)
        weights = lax.dynamic_slice_in_dim(probs, offset, stride, 2)
        return summed + jnp.einsum(
            "shp,spc->shc", weights, latents, preferred_element_type=jnp.float32
        )

    summed = lax.fori_loop(
        0, blocks_used, read_block, jnp.zeros((sequences, heads, latent_size), jnp.float32)
    )
    summed = (
        summed
        + prob_self.astype(jnp.float32)[..., None] * new_latent.astype(jnp.float32)[:, None, :]
    )
    return summed.astype(jnp.bfloat16)


def body(
    tokens,
    cache_latent,
    cache_rope,
    lengths,
    attn_gain,
    latent_gain,
    post_attn_gain,
    ffn_gain,
    post_ffn_gain,
    w_query,
    w_query_rot,
    w_latent,
    w_key_rot,
    w_key_up,
    w_value_up,
    w_out,
    route_logits,
    routes,
    w_gate,
    w_up,
    w_down,
):
    own_rows, width = tokens.shape
    tensor_ways = lax.axis_size("tp")
    expert_ways = lax.axis_size("ep")
    latent_size, local_heads, key_size = w_key_up.shape
    rot_size = w_key_rot.shape[1]
    value_size = w_value_up.shape[2]
    group = own_rows * tensor_ways
    scale = (key_size + rot_size) ** (-0.5)
    inner = 2
    half_ways = tensor_ways // inner
    assert tensor_ways == half_ways * inner and half_ways == 2
    me = lax.axis_index("tp")
    low = me % inner

    def near(value):
        return lax.ppermute(value, "tp", [(i, i ^ 1) for i in range(tensor_ways)])

    def far(value):
        return lax.ppermute(value, "tp", [(i, i ^ inner) for i in range(tensor_ways)])

    def by_relation(value, axis):
        swapped = jnp.stack([lax.index_in_dim(value, s ^ 1, axis, False) for s in range(4)], axis)
        value = jnp.where(low == 1, swapped, value)
        swapped = jnp.stack([lax.index_in_dim(value, s ^ 2, axis, False) for s in range(4)], axis)
        return jnp.where(me >= inner, swapped, value)

    def exchange(blocks):
        one = near(blocks[1])
        two, three = far(jnp.stack([blocks[2], blocks[3]]))
        return [blocks[0], one, two, near(three)]

    from_far = far(tokens)
    row_blocks = [tokens, near(tokens), from_far, near(from_far)]
    group_tokens = jnp.concatenate(row_blocks, axis=0)
    group_rows = rms_scale(group_tokens.astype(jnp.float32), attn_gain).astype(jnp.bfloat16)
    key_raw = jnp.dot(
        group_rows[:own_rows], w_key_rot, preferred_element_type=jnp.float32
    ).astype(jnp.bfloat16)
    stacked = jnp.concatenate([w_query, w_query_rot, w_latent], axis=1)
    projected = jnp.dot(group_rows, stacked, preferred_element_type=jnp.float32).astype(
        jnp.bfloat16
    )
    plain_cols = local_heads * key_size
    rotary_cols = local_heads * rot_size
    latent_cols = local_heads * latent_size
    query_plain = projected[:, :plain_cols].reshape(group, local_heads, key_size)
    query_latent = jnp.einsum(
        "ghn,chn->ghc", query_plain, w_key_up, preferred_element_type=jnp.float32
    ).astype(jnp.bfloat16)
    packed = jnp.concatenate(
        [query_latent.reshape(group, latent_cols), projected[:, plain_cols:]], axis=1
    )
    packed = packed.reshape(tensor_ways, own_rows, packed.shape[1])
    packed = jnp.stack(exchange([packed[s] for s in range(tensor_ways)]), axis=1)
    heads = tensor_ways * local_heads
    query_latent = packed[:, :, :latent_cols].reshape(own_rows, heads, latent_size)
    query_rotary = packed[:, :, latent_cols : latent_cols + rotary_cols].reshape(
        own_rows, heads, rot_size
    )
    latent_raw = by_relation(packed[:, :, latent_cols + rotary_cols :], 1).reshape(
        own_rows, latent_size
    )
    positions = lengths.astype(jnp.float32)
    new_latent = rms_scale(latent_raw.astype(jnp.float32), latent_gain).astype(jnp.bfloat16)
    new_rope = rotate(key_raw.astype(jnp.float32), positions).astype(jnp.bfloat16)
    query_turned = rotate(query_rotary.astype(jnp.float32), positions[:, None]).astype(jnp.bfloat16)
    head_latent = attend(
        query_latent, query_turned, cache_latent, cache_rope, new_latent, new_rope, lengths, scale
    )
    head_blocks = head_latent.reshape(own_rows, tensor_ways, local_heads, latent_size)
    head_blocks = jnp.concatenate(
        exchange([head_blocks[:, s] for s in range(tensor_ways)]), axis=0
    )
    values = jnp.einsum("ghc,chv->ghv", head_blocks, w_value_up, preferred_element_type=jnp.float32)
    values = values.astype(jnp.bfloat16).reshape(group, local_heads * value_size)
    partial_attn = jnp.dot(values, w_out, preferred_element_type=jnp.float32)
    partial_attn = partial_attn.reshape(tensor_ways, own_rows, width)
    given = jnp.stack([partial_attn[1], partial_attn[3]]).astype(jnp.bfloat16)
    kept = jnp.stack([partial_attn[0], partial_attn[2]])
    half_sum = (kept + near(given).astype(jnp.float32)).astype(jnp.bfloat16)
    attn = half_sum.astype(jnp.float32) + far(half_sum)[::-1].astype(jnp.float32)
    token_half = jnp.stack([row_blocks[0], row_blocks[2]]).astype(jnp.float32)
    attn = attn.reshape(half_ways * own_rows, width).astype(jnp.bfloat16)
    mixed = (
        token_half.reshape(half_ways * own_rows, width)
        + rms_scale(attn.astype(jnp.float32), post_attn_gain)
    ).astype(jnp.bfloat16)
    ffn_input = rms_scale(mixed.astype(jnp.float32), ffn_gain).astype(jnp.bfloat16)
    mixed = mixed[:own_rows]
    half_width = width // inner
    left, right = ffn_input[:, :half_width], ffn_input[:, half_width:]
    own_cols = jnp.where(low == 0, left, right)
    other_cols = near(jnp.where(low == 0, right, left))
    top_k = routes.shape[1]
    capacity = (group * top_k + expert_ways - 1) // expert_ways + 1
    flat_routes = routes.reshape(-1)
    onehot = (flat_routes[:, None] == jnp.arange(expert_ways, dtype=jnp.int32)[None, :]).astype(
        jnp.int32
    )
    rank = jnp.sum((jnp.cumsum(onehot, axis=0) - onehot) * onehot, axis=1)
    slot_of = (flat_routes * capacity + rank).reshape(tensor_ways, own_rows, top_k)
    slot_of = by_relation(slot_of, 0)
    slot_ids = jnp.arange(expert_ways * capacity, dtype=jnp.int32)
    hits = slot_of[:, :, :, None] == slot_ids[None, None, None, :]
    dispatch_map = jnp.any(hits, axis=2).astype(jnp.bfloat16)
    map_own = jnp.concatenate([dispatch_map[0], dispatch_map[2]], axis=0)
    map_other = jnp.concatenate([dispatch_map[1], dispatch_map[3]], axis=0)
    slots = jnp.einsum(
        "gs,gd->sd",
        jnp.concatenate([map_own, map_other], axis=0),
        jnp.concatenate([own_cols, other_cols], axis=0),
        preferred_element_type=jnp.float32,
    )
    sent = slots.astype(jnp.bfloat16).reshape(expert_ways, capacity, half_width)
    arrived = lax.all_to_all(sent, "ep", split_axis=0, concat_axis=0, tiled=True)
    flat = arrived.reshape(expert_ways * capacity, half_width)
    partner = near(flat)
    first = jnp.where(low == 0, flat, partner)
    second = jnp.where(low == 0, partner, flat)
    flat = jnp.concatenate([first, second], axis=1)
    gate = jnp.minimum(jnp.dot(flat, w_gate[0], preferred_element_type=jnp.float32), clamp_limit)
    upward = jnp.clip(
        jnp.dot(flat, w_up[0], preferred_element_type=jnp.float32), -clamp_limit, clamp_limit
    )
    active = ((upward + 1.0) * gate * jax.nn.sigmoid(sigmoid_alpha * gate)).astype(jnp.bfloat16)
    partial_out = jnp.dot(active, w_down[0], preferred_element_type=jnp.float32)
    left, right = partial_out[:, :half_width], partial_out[:, half_width:]
    received = near(jnp.where(low == 0, right, left).astype(jnp.bfloat16))
    summed = (jnp.where(low == 0, left, right) + received.astype(jnp.float32)).astype(jnp.bfloat16)
    summed = summed.reshape(expert_ways, capacity, half_width)
    returned = lax.all_to_all(summed, "ep", split_axis=0, concat_axis=0, tiled=True)
    route_weights = jax.nn.softmax(route_logits, axis=-1).reshape(tensor_ways, own_rows, top_k)
    route_weights = by_relation(route_weights, 0)
    combine = jnp.sum(jnp.where(hits, route_weights[..., None], 0.0), axis=2)
    moe_part = jnp.dot(
        combine.reshape(group, -1),
        returned.reshape(-1, half_width).astype(jnp.float32),
        precision=lax.Precision.HIGHEST,
    )
    rows_half = inner * own_rows
    moe_half = moe_part[:rows_half] + far(moe_part[rows_half:].astype(jnp.bfloat16)).astype(
        jnp.float32
    )
    moe_half = moe_half.astype(jnp.bfloat16)
    mine, other = moe_half[:own_rows], near(moe_half[own_rows:])
    moe = jnp.concatenate(
        [jnp.where(low == 0, mine, other), jnp.where(low == 0, other, mine)], axis=1
    )
    result = (mixed.astype(jnp.float32) + rms_scale(moe.astype(jnp.float32), post_ffn_gain)).astype(
        jnp.bfloat16
    )
    return (result, new_latent, new_rope)


def solution(mesh):
    return jax.shard_map(
        body,
        mesh=mesh,
        in_specs=(
            P(("ep", "tp"), None),
            P(("ep", "tp"), None, None),
            P(("ep", "tp"), None, None),
            P(("ep", "tp")),
            P(),
            P(),
            P(),
            P(),
            P(),
            P(None, "tp"),
            P(None, "tp"),
            P(None, "tp"),
            P(),
            P(None, "tp", None),
            P(None, "tp", None),
            P("tp", None),
            P("ep", None),
            P("ep", None),
            P("ep", None, "tp"),
            P("ep", None, "tp"),
            P("ep", "tp", None),
        ),
        out_specs=(P(("ep", "tp"), None), P(("ep", "tp"), None), P(("ep", "tp"), None)),
        check_vma=False,
    )
```

```python
import jax
import jax.numpy as jnp
from jax import lax
from jax.experimental import pallas as pl
from jax.experimental.pallas import tpu as pltpu
from jax.sharding import PartitionSpec as P

eps_norm = 1e-06
clamp_limit = 7.0
sigmoid_alpha = 1.702
theta_base = 10000.0


def rms_scale(values, gain):
    mean_square = jnp.mean(values * values, axis=-1, keepdims=True)
    return values * lax.rsqrt(mean_square + eps_norm) * gain.astype(jnp.float32)


def rotate(values, positions):
    half = values.shape[-1] // 2
    freqs = theta_base ** (-jnp.arange(half, dtype=jnp.float32) / half)
    angles = positions[..., None] * freqs
    cosine = jnp.cos(angles)
    sine = jnp.sin(angles)
    first = values[..., :half]
    second = values[..., half:]
    return jnp.concatenate(
        [first * cosine - second * sine, second * cosine + first * sine], axis=-1
    )


def attend(
    query_latent, query_turned, cache_latent, cache_rope, new_latent, new_rope, lengths, scale
):
    sequences, heads, latent_size = query_latent.shape
    span = cache_latent.shape[1]
    rot_size = cache_rope.shape[1]
    stride = min(256, span)
    assert span % stride == 0
    pieces = span // stride
    together = 4 if sequences % 4 == 0 else 1

    def kernel(
        lengths_ref,
        query_ref,
        turned_ref,
        fresh_ref,
        fresh_rope_ref,
        latent_hbm,
        rope_hbm,
        out_ref,
        latent_buf,
        rope_buf,
        latent_sems,
        rope_sems,
    ):
        def copies(row, piece):
            part = pl.ds(piece * stride, stride)
            return (
                pltpu.make_async_copy(
                    latent_hbm.at[row, part], latent_buf.at[row, part], latent_sems.at[row, piece]
                ),
                pltpu.make_async_copy(
                    rope_hbm.at[row, :, part],
                    rope_buf.at[row, :, part],
                    rope_sems.at[row, piece],
                ),
            )

        def used(row):
            return jnp.maximum((lengths_ref[row] + stride - 1) // stride, 1)

        def start(row, carry):
            count = used(row)
            for piece in range(pieces):

                @pl.when(piece < count)
                def _():
                    for copy in copies(row, piece):
                        copy.start()

            return carry

        lax.fori_loop(0, sequences, start, 0)

        def clear(row, carry):
            count = used(row)
            for piece in range(1, pieces):

                @pl.when(piece >= count)
                def _():
                    latent_buf[row, piece * stride : (piece + 1) * stride, :] = jnp.zeros(
                        (stride, latent_size), latent_buf.dtype
                    )

            return carry

        lax.fori_loop(0, sequences, clear, 0)

        def several(first, size):
            rows = [first + offset for offset in range(together)]
            width = size * stride
            spans = [slice(piece * stride, (piece + 1) * stride) for piece in range(size)]
            places = lax.broadcasted_iota(jnp.int32, (heads, width), 1)
            all_scores = []
            for row in rows:
                query = query_ref[row]
                turned = turned_ref[row]
                parts = [
                    lax.dot_general(
                        query,
                        latent_buf[row, part, :],
                        (((1,), (1,)), ((), ())),
                        preferred_element_type=jnp.float32,
                    )
                    + jnp.dot(
                        turned, rope_buf[row, :, part], preferred_element_type=jnp.float32
                    )
                    for part in spans
                ]
                all_scores.append(jnp.concatenate(parts, axis=1))
            weights = []
            for row, scores in zip(rows, all_scores):
                query = query_ref[row].astype(jnp.float32)
                turned = turned_ref[row].astype(jnp.float32)
                own = jnp.sum(query * fresh_ref[row].astype(jnp.float32), axis=1, keepdims=True)
                own = own + jnp.sum(
                    turned * fresh_rope_ref[row].astype(jnp.float32), axis=1, keepdims=True
                )
                own = own * scale
                masked = jnp.where(places < lengths_ref[row], scores * scale, -jnp.inf)
                highest = jnp.maximum(jnp.max(masked, axis=1, keepdims=True), own)
                raised = jnp.exp(masked - highest)
                raised_own = jnp.exp(own - highest)
                inverse = 1.0 / (jnp.sum(raised, axis=1, keepdims=True) + raised_own)
                weights.append(
                    (
                        (raised * inverse).astype(jnp.bfloat16),
                        (raised_own * inverse).astype(jnp.bfloat16).astype(jnp.float32),
                    )
                )
            for row, (probs, prob_own) in zip(rows, weights):
                summed = prob_own * fresh_ref[row].astype(jnp.float32)
                for part in spans:
                    summed = summed + jnp.dot(
                        probs[:, part], latent_buf[row, part, :], preferred_element_type=jnp.float32
                    )
                out_ref[row] = summed.astype(out_ref.dtype)

        def step(index, carry):
            first = index * together
            most = used(first)
            for offset in range(together):
                row = first + offset
                count = used(row)
                most = jnp.maximum(most, count)
                for piece in range(pieces):

                    @pl.when(piece < count)
                    def _():
                        for copy in copies(row, piece):
                            copy.wait()

            for size in range(1, pieces + 1):

                @pl.when(most == size)
                def _():
                    several(first, size)

            return carry

        lax.fori_loop(0, sequences // together, step, 0)

    vmem = pl.BlockSpec(memory_space=pltpu.VMEM)
    hbm = pl.BlockSpec(memory_space=pl.ANY)
    return pl.pallas_call(
        kernel,
        out_shape=jax.ShapeDtypeStruct((sequences, heads, latent_size), jnp.bfloat16),
        in_specs=[pl.BlockSpec(memory_space=pltpu.SMEM), vmem, vmem, vmem, vmem, hbm, hbm],
        out_specs=vmem,
        scratch_shapes=[
            pltpu.VMEM((sequences, span, latent_size), cache_latent.dtype),
            pltpu.VMEM((sequences, rot_size, span), cache_rope.dtype),
            pltpu.SemaphoreType.DMA((sequences, pieces)),
            pltpu.SemaphoreType.DMA((sequences, pieces)),
        ],
        compiler_params=pltpu.CompilerParams(vmem_limit_bytes=40 * 1024 * 1024),
        name="attend",
    )(
        lengths,
        query_latent,
        query_turned,
        new_latent[:, None, :],
        new_rope[:, None, :],
        cache_latent,
        cache_rope,
    )


def body(
    tokens,
    cache_latent,
    cache_rope,
    lengths,
    attn_gain,
    latent_gain,
    post_attn_gain,
    ffn_gain,
    post_ffn_gain,
    w_query,
    w_query_rot,
    w_latent,
    w_key_rot,
    w_key_up,
    w_value_up,
    w_out,
    route_logits,
    routes,
    w_gate,
    w_up,
    w_down,
):
    own_rows, width = tokens.shape
    tensor_ways = lax.axis_size("tp")
    expert_ways = lax.axis_size("ep")
    latent_size, local_heads, key_size = w_key_up.shape
    rot_size = w_key_rot.shape[1]
    value_size = w_value_up.shape[2]
    group = own_rows * tensor_ways
    scale = (key_size + rot_size) ** (-0.5)
    inner = 2
    half_ways = tensor_ways // inner
    assert tensor_ways == half_ways * inner and half_ways == 2
    me = lax.axis_index("tp")
    low = me % inner

    def near(value):
        return lax.ppermute(value, "tp", [(i, i ^ 1) for i in range(tensor_ways)])

    def far(value):
        return lax.ppermute(value, "tp", [(i, i ^ inner) for i in range(tensor_ways)])

    def by_relation(value, axis):
        swapped = jnp.stack([lax.index_in_dim(value, s ^ 1, axis, False) for s in range(4)], axis)
        value = jnp.where(low == 1, swapped, value)
        swapped = jnp.stack([lax.index_in_dim(value, s ^ 2, axis, False) for s in range(4)], axis)
        return jnp.where(me >= inner, swapped, value)

    def exchange(blocks):
        one = near(blocks[1])
        two, three = far(jnp.stack([blocks[2], blocks[3]]))
        return [blocks[0], one, two, near(three)]

    from_far = far(tokens)
    row_blocks = [tokens, near(tokens), from_far, near(from_far)]
    group_tokens = jnp.concatenate(row_blocks, axis=0)
    group_rows = rms_scale(group_tokens.astype(jnp.float32), attn_gain).astype(jnp.bfloat16)
    key_raw = jnp.dot(
        group_rows[:own_rows], w_key_rot, preferred_element_type=jnp.float32
    ).astype(jnp.bfloat16)
    stacked = jnp.concatenate([w_query, w_query_rot, w_latent], axis=1)
    projected = jnp.dot(group_rows, stacked, preferred_element_type=jnp.float32).astype(
        jnp.bfloat16
    )
    plain_cols = local_heads * key_size
    rotary_cols = local_heads * rot_size
    latent_cols = local_heads * latent_size
    query_plain = projected[:, :plain_cols].reshape(group, local_heads, key_size)
    query_latent = jnp.einsum(
        "ghn,chn->ghc", query_plain, w_key_up, preferred_element_type=jnp.float32
    ).astype(jnp.bfloat16)
    packed = jnp.concatenate(
        [query_latent.reshape(group, latent_cols), projected[:, plain_cols:]], axis=1
    )
    packed = packed.reshape(tensor_ways, own_rows, packed.shape[1])
    packed = jnp.stack(exchange([packed[s] for s in range(tensor_ways)]), axis=1)
    heads = tensor_ways * local_heads
    query_latent = packed[:, :, :latent_cols].reshape(own_rows, heads, latent_size)
    query_rotary = packed[:, :, latent_cols : latent_cols + rotary_cols].reshape(
        own_rows, heads, rot_size
    )
    latent_raw = by_relation(packed[:, :, latent_cols + rotary_cols :], 1).reshape(
        own_rows, latent_size
    )
    positions = lengths.astype(jnp.float32)
    new_latent = rms_scale(latent_raw.astype(jnp.float32), latent_gain).astype(jnp.bfloat16)
    new_rope = rotate(key_raw.astype(jnp.float32), positions).astype(jnp.bfloat16)
    query_turned = rotate(query_rotary.astype(jnp.float32), positions[:, None]).astype(jnp.bfloat16)
    head_latent = attend(
        query_latent, query_turned, cache_latent, cache_rope, new_latent, new_rope, lengths, scale
    )
    head_blocks = head_latent.reshape(own_rows, tensor_ways, local_heads, latent_size)
    head_blocks = jnp.concatenate(
        exchange([head_blocks[:, s] for s in range(tensor_ways)]), axis=0
    )
    values = jnp.einsum("ghc,chv->ghv", head_blocks, w_value_up, preferred_element_type=jnp.float32)
    values = values.astype(jnp.bfloat16).reshape(group, local_heads * value_size)
    partial_attn = jnp.dot(values, w_out, preferred_element_type=jnp.float32)
    partial_attn = partial_attn.reshape(tensor_ways, own_rows, width)
    given = jnp.stack([partial_attn[1], partial_attn[3]]).astype(jnp.bfloat16)
    kept = jnp.stack([partial_attn[0], partial_attn[2]])
    half_sum = (kept + near(given).astype(jnp.float32)).astype(jnp.bfloat16)
    attn = half_sum.astype(jnp.float32) + far(half_sum)[::-1].astype(jnp.float32)
    token_half = jnp.stack([row_blocks[0], row_blocks[2]]).astype(jnp.float32)
    attn = attn.reshape(half_ways * own_rows, width).astype(jnp.bfloat16)
    mixed = (
        token_half.reshape(half_ways * own_rows, width)
        + rms_scale(attn.astype(jnp.float32), post_attn_gain)
    ).astype(jnp.bfloat16)
    ffn_input = rms_scale(mixed.astype(jnp.float32), ffn_gain).astype(jnp.bfloat16)
    mixed = mixed[:own_rows]
    half_width = width // inner
    left, right = ffn_input[:, :half_width], ffn_input[:, half_width:]
    own_cols = jnp.where(low == 0, left, right)
    other_cols = near(jnp.where(low == 0, right, left))
    top_k = routes.shape[1]
    capacity = (group * top_k + expert_ways - 1) // expert_ways + 1
    flat_routes = routes.reshape(-1)
    onehot = (flat_routes[:, None] == jnp.arange(expert_ways, dtype=jnp.int32)[None, :]).astype(
        jnp.int32
    )
    rank = jnp.sum((jnp.cumsum(onehot, axis=0) - onehot) * onehot, axis=1)
    slot_of = (flat_routes * capacity + rank).reshape(tensor_ways, own_rows, top_k)
    slot_of = by_relation(slot_of, 0)
    slot_ids = jnp.arange(expert_ways * capacity, dtype=jnp.int32)
    hits = slot_of[:, :, :, None] == slot_ids[None, None, None, :]
    dispatch_map = jnp.any(hits, axis=2).astype(jnp.bfloat16)
    map_own = jnp.concatenate([dispatch_map[0], dispatch_map[2]], axis=0)
    map_other = jnp.concatenate([dispatch_map[1], dispatch_map[3]], axis=0)
    slots = jnp.einsum(
        "gs,gd->sd",
        jnp.concatenate([map_own, map_other], axis=0),
        jnp.concatenate([own_cols, other_cols], axis=0),
        preferred_element_type=jnp.float32,
    )
    sent = slots.astype(jnp.bfloat16).reshape(expert_ways, capacity, half_width)
    arrived = lax.all_to_all(sent, "ep", split_axis=0, concat_axis=0, tiled=True)
    flat = arrived.reshape(expert_ways * capacity, half_width)
    partner = near(flat)
    first = jnp.where(low == 0, flat, partner)
    second = jnp.where(low == 0, partner, flat)
    flat = jnp.concatenate([first, second], axis=1)
    gate = jnp.minimum(jnp.dot(flat, w_gate[0], preferred_element_type=jnp.float32), clamp_limit)
    upward = jnp.clip(
        jnp.dot(flat, w_up[0], preferred_element_type=jnp.float32), -clamp_limit, clamp_limit
    )
    active = ((upward + 1.0) * gate * jax.nn.sigmoid(sigmoid_alpha * gate)).astype(jnp.bfloat16)
    partial_out = jnp.dot(active, w_down[0], preferred_element_type=jnp.float32).astype(
        jnp.bfloat16
    )
    left, right = partial_out[:, :half_width], partial_out[:, half_width:]
    received = near(jnp.where(low == 0, right, left)).astype(jnp.float32)
    summed = jnp.where(low == 0, left, right).astype(jnp.float32) + received
    summed = summed.astype(jnp.bfloat16)
    summed = summed.reshape(expert_ways, capacity, half_width)
    returned = lax.all_to_all(summed, "ep", split_axis=0, concat_axis=0, tiled=True)
    route_weights = jax.nn.softmax(route_logits, axis=-1).reshape(tensor_ways, own_rows, top_k)
    route_weights = by_relation(route_weights, 0)
    combine = jnp.sum(jnp.where(hits, route_weights[..., None], 0.0), axis=2)
    moe_part = jnp.dot(
        combine.reshape(group, -1),
        returned.reshape(-1, half_width).astype(jnp.float32),
        precision=lax.Precision.HIGHEST,
    )
    rows_half = inner * own_rows
    moe_half = moe_part[:rows_half] + far(moe_part[rows_half:].astype(jnp.bfloat16)).astype(
        jnp.float32
    )
    moe_half = moe_half.astype(jnp.bfloat16)
    mine, other = moe_half[:own_rows], near(moe_half[own_rows:])
    moe = jnp.concatenate(
        [jnp.where(low == 0, mine, other), jnp.where(low == 0, other, mine)], axis=1
    )
    result = (mixed.astype(jnp.float32) + rms_scale(moe.astype(jnp.float32), post_ffn_gain)).astype(
        jnp.bfloat16
    )
    return (result, new_latent, new_rope)


def solution(mesh):
    return jax.shard_map(
        body,
        mesh=mesh,
        in_specs=(
            P(("ep", "tp"), None),
            P(("ep", "tp"), None, None),
            P(("ep", "tp"), None, None),
            P(("ep", "tp")),
            P(),
            P(),
            P(),
            P(),
            P(),
            P(None, "tp"),
            P(None, "tp"),
            P(None, "tp"),
            P(),
            P(None, "tp", None),
            P(None, "tp", None),
            P("tp", None),
            P("ep", None),
            P("ep", None),
            P("ep", None, "tp"),
            P("ep", None, "tp"),
            P("ep", "tp", None),
        ),
        out_specs=(P(("ep", "tp"), None), P(("ep", "tp"), None), P(("ep", "tp"), None)),
        check_vma=False,
    )
```
